128 devices in a mesh: sp: 16 (over z, y), dp: 8 (over x, core).
Axes of the slice: x: 4, y: 4, z: 4, core: 2. Of those that a mesh axis runs over, the one named last changes fastest.
Arguments:
- layer_input: bfloat16 [8, 2048, 2048], P('dp', 'sp'), may hold values from -0.0390625 to 0.0390625
- queries: bfloat16 [8, 2048, 2048], P('dp', 'sp'), may hold values from -6 to 6
- key_vectors: bfloat16 [8, 2048, 2048], P('dp', 'sp'), may hold values from -6 to 6
- values: bfloat16 [8, 2048, 4096], P('dp', 'sp'), may hold values from -6 to 6
- cotangent: bfloat16 [8, 2048, 4096], P('dp', 'sp'), may hold values from -0.3125 to 0.3125
- log_decay: float32 [8, 16, 2048], P('dp', 'sp'), may hold values from -3 to 0
- key_weight: bfloat16 [2048, 2048], P('dp'), may hold values from -0.125 to 0.125
Outputs:
- grad_query: bfloat16 [8, 2048, 2048], P('dp', 'sp')
- grad_value: bfloat16 [8, 2048, 4096], P('dp', 'sp')
- grad_input: bfloat16 [8, 2048, 2048], P('dp', 'sp')
- grad_key_weight: float32 [2048, 2048], P('dp')
The draws below stay inside these ranges and needn't reach their ends.
All inputs are finite; a program needn't handle non-finite values.
Results may differ from the reference program's by a relative error of at most 0.012.
Values may be sent and summed in bfloat16 or wider, within the bound.
A program may use at most 128 MiB of HBM per device.

```python
import jax
import jax.numpy as jnp
from jax import lax

D = 2048
HEADS = 8
DK = 256
DV = 512
BLOCK = 128
TOK_DEV = 128
HEAD_DIRECTIONS = 16
SEQUENCE_LENGTH = 2048
SEQUENCE_COUNT = 8
HK = 2048
HV = 4096


def draw_log_decay(key, part):
    parallel_lanes = jax.random.split(jax.random.fold_in(key, 71), 6)
    fast_share = 0.5
    is_fast = jax.random.uniform(parallel_lanes[0], (SEQUENCE_COUNT, HEAD_DIRECTIONS, 1)) < fast_share
    fast_rate = jnp.exp(jax.random.uniform(parallel_lanes[1], (SEQUENCE_COUNT, HEAD_DIRECTIONS, 1), jnp.float32, jnp.log(2.0), jnp.log(6.0))) / BLOCK
    slow_rate = jnp.ones((SEQUENCE_COUNT, HEAD_DIRECTIONS, 1), jnp.float32) / SEQUENCE_LENGTH
    baseline_decay_rate = jnp.where(is_fast, fast_rate, slow_rate)
    block_multiplier = jnp.exp(jax.random.uniform(parallel_lanes[2], (SEQUENCE_COUNT, HEAD_DIRECTIONS, SEQUENCE_LENGTH // TOK_DEV), jnp.float32, jnp.log(0.5), jnp.log(2.0)))
    block_multiplier = jnp.repeat(block_multiplier, TOK_DEV, axis=2)
    decay_jitter = jax.random.uniform(parallel_lanes[3], (SEQUENCE_COUNT, HEAD_DIRECTIONS, SEQUENCE_LENGTH), jnp.float32, 0.5, 1.5)
    group_position = jax.random.randint(parallel_lanes[4], (SEQUENCE_COUNT, HEAD_DIRECTIONS, 2), 0, SEQUENCE_LENGTH)
    group_depth = jnp.log(jax.random.uniform(parallel_lanes[5], (SEQUENCE_COUNT, HEAD_DIRECTIONS, 2), jnp.float32, 0.5, 0.8))
    position_slots = jnp.arange(SEQUENCE_LENGTH)[None, None, None, :]
    token_groups = jnp.sum(jnp.where(position_slots == group_position[..., None], group_depth[..., None], 0.0), axis=2)
    return (-baseline_decay_rate * block_multiplier * decay_jitter + token_groups).astype(jnp.float32)


def with_spikes(drawn, own_key, source, target, blocks, factor):
    def block_of(axis_at):
        return (jnp.arange(drawn.shape[axis_at]) // (drawn.shape[axis_at] // blocks)).reshape((-1,) + (1,) * (drawn.ndim - 1 - axis_at))

    near = jax.random.permutation(own_key, blocks)[block_of(target)]
    other_side = (block_of(target) + blocks // 2) % blocks
    return jnp.where((block_of(source) == near) | (block_of(source) == other_side), factor * drawn, drawn)


def level_of(rng, shape, cuts, least, largest):
    loudness, own = 1.0, jax.random.fold_in(rng, 6)
    for dim, shards_of in cuts:
        draws = jnp.exp(jax.random.uniform(jax.random.fold_in(own, dim), (shards_of,), jnp.float32, least / len(cuts), largest / len(cuts)))
        loudness = loudness * jnp.repeat(draws, shape[dim] // shards_of).reshape([-1 if axis == dim else 1 for axis in range(len(shape))])
    return loudness


def scatter_about(rng, dims, scale, reach, cuts=(), held_as=jnp.bfloat16):
    gain = level_of(rng, dims, cuts, -0.22, 0.18) if cuts else 1.0
    drawn = jax.random.normal(rng, dims, jnp.float32) * scale * gain
    return jnp.minimum(jnp.maximum(drawn, -reach), reach).astype(held_as)


def heavy_noise(own_key, shape, width, most, shards, heavy, kind=jnp.bfloat16):
    values = width * jax.random.normal(own_key, shape, jnp.float32)
    if shards:
        values = values * level_of(own_key, shape, shards, -0.22, 0.18)
    return jnp.clip(with_spikes(values, jax.random.fold_in(own_key, 3), *heavy), -most, most).astype(kind)


def setup_inputs(seed: int = 0) -> dict:
    streams_of = jax.random.split(jax.random.key(seed), 8)
    layer_input = heavy_noise(streams_of[0], (SEQUENCE_COUNT, SEQUENCE_LENGTH, D), 0.005, 0.0390625, ((0, 8), (1, 16)), (1, 2, 16, 2.0))
    queries = scatter_about(streams_of[1], (SEQUENCE_COUNT, SEQUENCE_LENGTH, HK), 1.0, 6.0, ((0, 8), (1, 16)))
    key_vectors = scatter_about(streams_of[2], (SEQUENCE_COUNT, SEQUENCE_LENGTH, HK), 1.0, 6.0, ((0, 8), (1, 16)))
    values = scatter_about(streams_of[3], (SEQUENCE_COUNT, SEQUENCE_LENGTH, HV), 1.0, 6.0, ((0, 8), (1, 16)))
    cotangent = scatter_about(streams_of[4], (SEQUENCE_COUNT, SEQUENCE_LENGTH, HV), 0.05, 0.3125, ((0, 8), (1, 16)))
    log_decay = draw_log_decay(jax.random.fold_in(streams_of[7], 71), 0)
    key_weight = scatter_about(streams_of[6], (D, HK), D ** -0.5, 0.125, ((0, 8),))
    return {"layer_input": layer_input, "queries": queries, "key_vectors": key_vectors, "values": values, "cotangent": cotangent, "log_decay": log_decay, "key_weight": key_weight}


def unit_backward(query_rows, key_rows, value_rows, grad_rows, decay_rows, strict):
    length, key_width = query_rows.shape
    value_width = value_rows.shape[1]
    blocks = length // BLOCK
    scaling = key_width ** -0.5
    query_blk = query_rows.reshape(blocks, BLOCK, key_width)
    key_blk = key_rows.reshape(blocks, BLOCK, key_width)
    value_blk = value_rows.reshape(blocks, BLOCK, value_width)
    grad_blk = grad_rows.reshape(blocks, BLOCK, value_width)
    within = jnp.cumsum(decay_rows.reshape(blocks, BLOCK), axis=1)
    position_slots = jnp.arange(BLOCK)
    allowed = jnp.where(strict, position_slots[None, :] < position_slots[:, None], position_slots[None, :] <= position_slots[:, None])
    spread = jnp.where(allowed, within[:, :, None] - within[:, None, :], 0.0)
    weights = jnp.where(allowed, jnp.exp(spread), 0.0) * scaling
    raw_scores = jnp.einsum("nid,njd->nij", query_blk, key_blk, preferred_element_type=jnp.float32)
    scores = (raw_scores * weights).astype(jnp.bfloat16)
    raw_grads = jnp.einsum("niv,njv->nij", grad_blk, value_blk, preferred_element_type=jnp.float32)
    grad_scores = (raw_grads * weights).astype(jnp.bfloat16)
    value_inner = jnp.einsum("nij,niv->njv", scores, grad_blk, preferred_element_type=jnp.float32)
    query_inner = jnp.einsum("nij,njd->nid", grad_scores, key_blk, preferred_element_type=jnp.float32)
    key_inner = jnp.einsum("nij,nid->njd", grad_scores, query_blk, preferred_element_type=jnp.float32)
    ending = within[:, -1:]
    query_scale = jnp.exp(within) * scaling
    key_scale = jnp.exp(ending - within)
    carry_decay = jnp.exp(ending[:, 0])
    query_dec = (query_blk * query_scale[:, :, None]).astype(jnp.bfloat16)
    key_dec = (key_blk * key_scale[:, :, None]).astype(jnp.bfloat16)
    contract = (((0,), (0,)), ((), ()))

    def advance(memory, inputs):
        key_b, value_b, factor = inputs
        before = memory.astype(jnp.bfloat16)
        memory = factor * memory + lax.dot_general(key_b, value_b, contract, preferred_element_type=jnp.float32)
        return memory, before

    start_state = jnp.zeros((key_width, value_width), jnp.float32)
    _, states_before = lax.scan(advance, start_state, (key_dec, value_blk, carry_decay))

    def retreat(later, inputs):
        query_b, grad_b, factor = inputs
        after = later.astype(jnp.bfloat16)
        later = factor * later + lax.dot_general(query_b, grad_b, contract, preferred_element_type=jnp.float32)
        return later, after

    _, state_grads = lax.scan(retreat, start_state, (query_dec, grad_blk, carry_decay), reverse=True)
    query_carried = jnp.einsum("niv,ndv->nid", grad_blk, states_before, preferred_element_type=jnp.float32)
    key_carried = jnp.einsum("njv,ndv->njd", value_blk, state_grads, preferred_element_type=jnp.float32)
    value_carried = jnp.einsum("njd,ndv->njv", key_dec, state_grads, preferred_element_type=jnp.float32)
    grad_q = query_inner + query_carried * query_scale[:, :, None]
    grad_k = key_inner + key_carried * key_scale[:, :, None]
    grad_v = value_inner + value_carried
    return (grad_q.reshape(length, key_width), grad_k.reshape(length, key_width),
            grad_v.reshape(length, value_width))


def unit_grads(query_rows, key_rows, value_rows, grad_rows, decay_rows, backward):
    def orient(array):
        return jnp.where(backward, jnp.flip(array, 0), array)

    gradients = unit_backward(orient(query_rows), orient(key_rows), orient(value_rows),
                              orient(grad_rows), orient(decay_rows), backward)
    return tuple(orient(single).astype(jnp.bfloat16) for single in gradients)


def reference(layer_input, queries, key_vectors, values, cotangent, log_decay, key_weight):
    def one_sequence(inputs):
        rows_in, query_seq, key_seq, value_seq, grad_seq, decay_seq = inputs
        length = query_seq.shape[0]
        query_heads = query_seq.reshape(length, HEADS, DK)
        key_heads = key_seq.reshape(length, HEADS, DK)
        value_heads = value_seq.reshape(length, HEADS, DV)
        grad_heads = grad_seq.reshape(length, HEADS, DV)
        query_list, key_list, value_list = [], [], []
        for head_index in range(HEADS):
            halves = [unit_grads(query_heads[:, head_index], key_heads[:, head_index], value_heads[:, head_index],
                                 grad_heads[:, head_index], decay_seq[2 * head_index + direction], direction == 1)
                      for direction in range(2)]
            paired = [(halves[0][slot].astype(jnp.float32) + halves[1][slot].astype(jnp.float32)).astype(jnp.bfloat16)
                      for slot in range(3)]
            query_list.append(paired[0])
            key_list.append(paired[1])
            value_list.append(paired[2])
        grad_query = jnp.concatenate(query_list, axis=1)
        grad_key = jnp.concatenate(key_list, axis=1)
        grad_value = jnp.concatenate(value_list, axis=1)
        grad_input = jnp.dot(grad_key, key_weight.T, preferred_element_type=jnp.float32).astype(jnp.bfloat16)
        local_term = jnp.dot(rows_in.T, grad_key, preferred_element_type=jnp.float32)
        return grad_query, grad_value, grad_input, local_term

    outputs = lax.map(one_sequence, (layer_input, queries, key_vectors, values, cotangent, log_decay))
    return outputs[0], outputs[1], outputs[2], jnp.sum(outputs[3], axis=0)
```

```python
import functools

import jax
import jax.numpy as jnp
from jax import lax
from jax.experimental import pallas as pl
from jax.experimental.pallas import tpu as pltpu
from jax.sharding import PartitionSpec as P

F32 = jnp.float32
BF16 = jnp.bfloat16
SP, DPN = 16, 8
GROUP = 8
DK, DV, D = 256, 512, 2048
BLOCK = 128
MESH = pl.DeviceIdType.MESH


def dot(a, b, ca, cb, precision=None):
    return lax.dot_general(
        a, b, (((ca,), (cb,)), ((), ())), preferred_element_type=F32, precision=precision
    )


def lanes(scale, width):
    return jnp.concatenate([scale] * (width // 128), axis=1)


def kernel(
    x_ref, q_ref, k_ref, v_ref, g_ref, lam_ref, w_ref,
    dq_ref, dv_ref, dx_ref, dw_ref,
    rq, rk, rv, rg, rlam, w_all, x_all,
    qs, ks, ee, tails, wgt,
    acc_q, acc_k, acc_v, m_st, g_st, st_tx, st_rx,
    out_q, out_k, out_v, dk_all, dx_st, dw_acc, dw_tx, dw_rx, sum_tx, sum_rx,
    in_send, in_recv, lam_send, lam_recv, x_send, x_recv, w_sem,
    st_send, st_recv, out_send, out_recv, dk_send, dk_fwd, dk_recv,
    dx_send, dx_recv, rs_send, rs_recv, ag_send, ag_recv,
):
    s = lax.axis_index("sp")
    d = lax.axis_index("dp")
    gz = s // GROUP
    me = s % GROUP
    head = (me + 4 * gz) % GROUP
    base = GROUP * gz
    partner = GROUP * (1 - gz) + (head + 4 * (1 - gz)) % GROUP
    xi, core = d // 2, d % 2
    sibling = 2 * xi + 1 - core

    def col(i, width):
        return pl.ds(pl.multiple_of(i * width, width), width)

    def remote(src, dst, ssem, rsem, to):
        return pltpu.make_async_remote_copy(
            src_ref=src, dst_ref=dst, send_sem=ssem, recv_sem=rsem,
            device_id=to, device_id_type=MESH,
        )

    def arrived(dst, sem):
        pltpu.make_async_copy(dst, dst, sem).wait()

    barrier = pltpu.get_barrier_semaphore()

    @pl.loop(1, SP)
    def _(i):
        pl.semaphore_signal(barrier, inc=1, device_id=((s + i) % SP, d), device_id_type=MESH)

    @pl.loop(1, DPN)
    def _(i):
        pl.semaphore_signal(barrier, inc=1, device_id=(s, (d + i) % DPN), device_id_type=MESH)

    pl.semaphore_wait(barrier, SP + DPN - 2)

    lam_to = [s // 2, GROUP + (s // 2 + 4) % GROUP]
    for half in range(2):
        src = lam_ref.at[pl.ds(8 * half, 8), :]

        @pl.when(lam_to[half] == s)
        def _():
            pltpu.make_async_copy(src, rlam.at[s % 2], lam_recv.at[s % 2]).start()

        @pl.when(lam_to[half] != s)
        def _():
            remote(src, rlam.at[s % 2], lam_send.at[half], lam_recv.at[s % 2], (lam_to[half], d)).start()

    pairs = ((q_ref, rq, DK), (k_ref, rk, DK), (v_ref, rv, DV), (g_ref, rg, DV))
    for n, (src, dst, width) in enumerate(pairs):
        pltpu.make_async_copy(src.at[:, col(head, width)], dst.at[me], in_recv.at[n, me]).start()

    @pl.loop(1, GROUP)
    def _(i):
        to = (me + i) % GROUP
        its_head = (to + 4 * gz) % GROUP
        for n, (src, dst, width) in enumerate(pairs):
            remote(
                src.at[:, col(its_head, width)], dst.at[me],
                in_send.at[n, to], in_recv.at[n, me], (base + to, d),
            ).start()

    pltpu.make_async_copy(x_ref.at[:, col(d, 256)], x_all.at[d], x_recv.at[d]).start()

    @pl.loop(1, DPN)
    def _(i):
        to = (d + i) % DPN
        remote(x_ref.at[:, col(to, 256)], x_all.at[d], x_send.at[to], x_recv.at[d], (s, to)).start()

    w_copy = pltpu.make_async_copy(w_ref, w_all, w_sem)
    w_copy.start()

    for r in range(2):
        arrived(rlam.at[r], lam_recv.at[r])
    row = lax.broadcasted_iota(jnp.int32, (BLOCK, BLOCK), 0)
    column = lax.broadcasted_iota(jnp.int32, (BLOCK, BLOCK), 1)
    ones = jnp.ones((BLOCK, BLOCK), F32)
    hi = lax.Precision.HIGHEST

    @pl.loop(0, GROUP)
    def _(b):
        kept = []
        for r in range(2):
            lam = jnp.broadcast_to(rlam[r, pl.ds(b, 1), :], (BLOCK, BLOCK))
            seen = column <= row if r == 0 else column >= row
            c = dot(jnp.where(seen, lam, 0.0), ones, 1, 0, hi)
            kept.append(c - c.T)
            end = c[BLOCK - 1 : BLOCK, :] if r == 0 else c[0:1, :]
            qs[r, b] = jnp.exp(c) * 0.0625
            ks[r, b] = jnp.exp(end - c)
            ee[r, b] = jnp.broadcast_to(end, (8, 128))
        wgt[b] = jnp.exp(jnp.where(column <= row, kept[0], kept[1])) * 0.0625

    for r in range(2):
        up = jnp.zeros((8, 128), F32)
        down = jnp.zeros((8, 128), F32)
        for b in range(GROUP):
            tails[r, 1, b] = jnp.exp(down)
            down = down + ee[r, b]
            tails[r, 0, GROUP - 1 - b] = jnp.exp(up)
            up = up + ee[r, GROUP - 1 - b]
        for b in range(GROUP):
            ee[r, b] = jnp.exp(ee[r, b])

    m_st[...] = jnp.zeros_like(m_st)
    g_st[...] = jnp.zeros_like(g_st)

    @pl.loop(0, GROUP)
    def _(i):
        b = (me + GROUP - i) % GROUP
        for n, (_, dst, _) in enumerate(pairs):
            arrived(dst.at[b], in_recv.at[n, b])
        q, k, v, g = rq[b], rk[b], rv[b], rg[b]
        rm, rgr = gz, 1 - gz
        km = ks[rm, b] * tails[rm, gz, b][0:1, :]
        qg = qs[rgr, b] * tails[rgr, gz, b][0:1, :]
        m_st[...] += dot((k.astype(F32) * lanes(km, DK)).astype(BF16), v, 0, 0)
        g_st[...] += dot((q.astype(F32) * lanes(qg, DK)).astype(BF16), g, 0, 0)
        w = wgt[b]
        sc = (dot(q, k, 1, 1) * w).astype(BF16)
        gs = (dot(g, v, 1, 1) * w).astype(BF16)
        acc_v[b] = dot(sc, g, 0, 0)
        acc_q[b] = dot(gs, k, 1, 0)
        acc_k[b] = dot(gs, q, 0, 0)

    st_tx[0] = m_st[...].astype(BF16)
    st_tx[1] = g_st[...].astype(BF16)
    for n in range(2):
        remote(st_tx.at[n], st_rx.at[n], st_send.at[n], st_recv.at[n], (partner, d)).start()

    def step(b, way):
        rm, rgr = way, 1 - way
        q, k, v, g = rq[b], rk[b], rv[b], rg[b]
        kf = k.astype(F32)
        mb, gb = m_st[...].astype(BF16), g_st[...].astype(BF16)
        ksg = lanes(ks[rgr, b], DK)
        dq = dot(g, mb, 1, 1) * lanes(qs[rm, b], DK)
        dk = dot(v, gb, 1, 1) * ksg
        dv = dot((kf * ksg).astype(BF16), gb, 1, 0)
        kd = (kf * lanes(ks[rm, b], DK)).astype(BF16)
        qd = (q.astype(F32) * lanes(qs[rgr, b], DK)).astype(BF16)
        m_st[...] = m_st[...] * lanes(ee[rm, b][0:1, :], DV) + dot(kd, v, 0, 0)
        g_st[...] = g_st[...] * lanes(ee[rgr, b][0:1, :], DV) + dot(qd, g, 0, 0)
        return dq, dk, dv

    m_st[...] = jnp.zeros_like(m_st)
    g_st[...] = jnp.zeros_like(g_st)

    @pl.loop(0, GROUP)
    def _(i):
        b = i + gz * (GROUP - 1 - 2 * i)
        dq, dk, dv = step(b, gz)
        acc_q[b] += dq
        acc_k[b] += dk
        acc_v[b] += dv

    for n in range(2):
        arrived(st_rx.at[n], st_recv.at[n])
    m_st[...] = st_rx[0].astype(F32)
    g_st[...] = st_rx[1].astype(F32)

    homes = (
        (out_k, dk_all.at[d], DK),
        (out_q, dq_ref, DK),
        (out_v, dv_ref, DV),
    )

    def send_home(b, n):
        src, dst, width = homes[n]

        @pl.when(b == me)
        def _():
            pltpu.make_async_copy(src.at[b], dst.at[:, col(head, width)], out_recv.at[n, head]).start()

        @pl.when(b != me)
        def _():
            remote(
                src.at[b], dst.at[:, col(head, width)],
                out_send.at[n, b], out_recv.at[n, head], (base + b, d),
            ).start()

    @pl.loop(0, GROUP)
    def _(i):
        b = i + (1 - gz) * (GROUP - 1 - 2 * i)
        dq, dk, dv = step(b, 1 - gz)
        out_k[b] = (acc_k[b] + dk).astype(BF16)
        send_home(b, 0)
        out_q[b] = (acc_q[b] + dq).astype(BF16)
        out_v[b] = (acc_v[b] + dv).astype(BF16)

    @pl.loop(0, GROUP)
    def _(i):
        b = (me + i) % GROUP
        send_home(b, 1)
        send_home(b, 2)

    @pl.loop(0, GROUP)
    def _(h):
        arrived(out_k.at[h], out_recv.at[0, h])

    own = dk_all.at[d]
    remote(own, own, dk_send.at[sibling], dk_recv.at[d], (s, sibling)).start()
    for t in (1, 3, 2):
        to = 2 * ((xi + t) % 4) + core
        remote(own, own, dk_send.at[to], dk_recv.at[d], (s, to)).start()

    @pl.loop(0, DPN)
    def _(j):
        arrived(x_all.at[j], x_recv.at[j])

    w_copy.wait()
    dw_acc[...] = jnp.zeros_like(dw_acc)

    def take(j):
        dx_st[j] = dot(dk_all[j], w_all[...], 1, 1).astype(BF16)
        xt = x_all[j]

        @pl.loop(0, 4)
        def _(c):
            dw_acc[:, col(c, 512)] += dot(xt, dk_all[j, :, col(c, 512)], 0, 0)

    def give(j):
        remote(dx_st.at[j], dx_ref.at[:, col(d, 256)], dx_send.at[j], dx_recv.at[d], (s, j)).start()

    take(d)
    pltpu.make_async_copy(dx_st.at[d], dx_ref.at[:, col(d, 256)], dx_recv.at[d]).start()
    arrived(dk_all.at[sibling], dk_recv.at[sibling])
    take(sibling)
    give(sibling)

    @pl.loop(0, 3)
    def _(i):
        t = 1 + (2 * i) % 3
        near = 2 * ((xi + t) % 4) + core
        far = 2 * ((xi + t) % 4) + 1 - core
        arrived(dk_all.at[near], dk_recv.at[near])
        remote(dk_all.at[near], dk_all.at[near], dk_fwd.at[i], dk_recv.at[near], (s, sibling)).start()
        take(near)
        give(near)
        arrived(dk_all.at[far], dk_recv.at[far])
        take(far)
        give(far)

    for j in range(SP):
        dw_tx[j] = dw_acc[:, 128 * j : 128 * (j + 1)].astype(BF16)
    pltpu.make_async_copy(dw_tx.at[s], dw_rx.at[s], rs_recv.at[s]).start()

    @pl.loop(1, SP)
    def _(i):
        to = (s + i) % SP
        remote(dw_tx.at[to], dw_rx.at[s], rs_send.at[to], rs_recv.at[s], (to, d)).start()

    @pl.loop(0, SP)
    def _(j):
        arrived(dw_rx.at[j], rs_recv.at[j])

    total = dw_rx[0].astype(F32)
    for j in range(1, SP):
        total += dw_rx[j].astype(F32)
    sum_tx[...] = total.astype(BF16)
    pltpu.make_async_copy(sum_tx, sum_rx.at[s], ag_recv.at[s]).start()

    @pl.loop(1, SP)
    def _(i):
        to = (s + i) % SP
        remote(sum_tx, sum_rx.at[s], ag_send.at[to], ag_recv.at[s], (to, d)).start()

    @pl.loop(0, SP)
    def _(j):
        arrived(sum_rx.at[j], ag_recv.at[j])

    for j in range(SP):
        dw_ref[:, 128 * j : 128 * (j + 1)] = sum_rx[j].astype(F32)

    @pl.loop(0, GROUP)
    def _(h):
        arrived(out_q.at[h], out_recv.at[1, h])
        arrived(out_v.at[h], out_recv.at[2, h])

    @pl.loop(0, DPN)
    def _(j):
        arrived(dx_st.at[j], dx_recv.at[j])

    for half in range(2):

        @pl.when(lam_to[half] != s)
        def _():
            arrived(rlam.at[half], lam_send.at[half])

    @pl.loop(1, GROUP)
    def _(i):
        to = (me + i) % GROUP
        for n, (_, dst, _) in enumerate(pairs):
            arrived(dst.at[to], in_send.at[n, to])
        for n, (src, _, _) in enumerate(homes):
            arrived(src.at[to], out_send.at[n, to])

    @pl.loop(1, DPN)
    def _(i):
        to = (d + i) % DPN
        arrived(x_all.at[to], x_send.at[to])
        arrived(dx_st.at[to], dx_send.at[to])

    for n in range(2):
        arrived(st_tx.at[n], st_send.at[n])
    arrived(own, dk_send.at[sibling])
    for t in range(1, 4):
        arrived(own, dk_send.at[2 * ((xi + t) % 4) + core])
        arrived(own, dk_fwd.at[t - 1])

    @pl.loop(1, SP)
    def _(i):
        to = (s + i) % SP
        arrived(sum_tx, rs_send.at[to])
        arrived(sum_tx, ag_send.at[to])


def step(x, q, k, v, g, lam, w):
    vmem = pl.BlockSpec(memory_space=pltpu.VMEM)
    hbm = pl.BlockSpec(memory_space=pl.ANY)
    dma = pltpu.SemaphoreType.DMA
    v_ = pltpu.VMEM
    dq, dv, dx, dw = pl.pallas_call(
        kernel,
        out_shape=(
            jax.ShapeDtypeStruct((BLOCK, 2048), BF16),
            jax.ShapeDtypeStruct((BLOCK, 4096), BF16),
            jax.ShapeDtypeStruct((BLOCK, 2048), BF16),
            jax.ShapeDtypeStruct((256, 2048), F32),
        ),
        in_specs=[hbm, vmem, vmem, vmem, vmem, vmem, hbm],
        out_specs=(vmem,) * 4,
        scratch_shapes=[
            v_((8, BLOCK, DK), BF16), v_((8, BLOCK, DK), BF16),
            v_((8, BLOCK, DV), BF16), v_((8, BLOCK, DV), BF16),
            v_((2, 8, 128), F32), v_((256, 2048), BF16), v_((8, BLOCK, 256), BF16),
            v_((2, 8, BLOCK, 128), F32), v_((2, 8, BLOCK, 128), F32),
            v_((2, 8, 8, 128), F32), v_((2, 2, 8, 8, 128), F32), v_((8, BLOCK, 128), F32),
            v_((8, BLOCK, DK), F32), v_((8, BLOCK, DK), F32), v_((8, BLOCK, DV), F32),
            v_((DK, DV), F32), v_((DK, DV), F32), v_((2, DK, DV), BF16), v_((2, DK, DV), BF16),
            v_((8, BLOCK, DK), BF16), v_((8, BLOCK, DK), BF16), v_((8, BLOCK, DV), BF16),
            v_((8, BLOCK, 2048), BF16), v_((8, BLOCK, 256), BF16),
            v_((256, 2048), F32), v_((16, 256, 128), BF16), v_((16, 256, 128), BF16),
            v_((256, 128), BF16), v_((16, 256, 128), BF16),
            dma((4, 8)), dma((4, 8)), dma((2,)), dma((2,)), dma((8,)), dma((8,)), dma,
            dma((2,)), dma((2,)), dma((3, 8)), dma((3, 8)), dma((8,)), dma((3,)), dma((8,)),
            dma((8,)), dma((8,)), dma((16,)), dma((16,)), dma((16,)), dma((16,)),
        ],
        compiler_params=pltpu.CompilerParams(
            collective_id=0, has_side_effects=True, vmem_limit_bytes=60 * 1024 * 1024
        ),
    )(x[0], q[0], k[0], v[0], g[0], lam[0].reshape(16, 128), w)
    return dq[None], dv[None], dx[None], dw


def solution(mesh):
    tokens = P("dp", "sp", None)
    return jax.shard_map(
        step,
        mesh=mesh,
        in_specs=(tokens,) * 6 + (P("dp", None),),
        out_specs=(tokens, tokens, tokens, P("dp", None)),
        check_vma=False,
    )
```

```python
import functools

import jax
import jax.numpy as jnp
from jax import lax
from jax.experimental import pallas as pl
from jax.experimental.pallas import tpu as pltpu
from jax.sharding import PartitionSpec as P

F32 = jnp.float32
BF16 = jnp.bfloat16
SP, DPN = 16, 8
GROUP = 8
DK, DV, D = 256, 512, 2048
BLOCK = 128
CHUNKS = 4
CHUNK = D // CHUNKS
MESH = pl.DeviceIdType.MESH


def dot(a, b, ca, cb, precision=None):
    return lax.dot_general(
        a, b, (((ca,), (cb,)), ((), ())), preferred_element_type=F32, precision=precision
    )


def lanes(scale, width):
    return jnp.concatenate([scale] * (width // 128), axis=1)


def kernel(
    x_ref, q_ref, k_ref, v_ref, g_ref, lam_ref, w_ref,
    dq_ref, dv_ref, dx_ref, dw_ref,
    rq, rk, rv, rg, rlam, w_all, x_all,
    qs, ks, ee, tails, wgt,
    acc_q, gs_all, g_all, st, st_tx, st_rx, out_q, out_k, out_v,
    dk_all, dx_st, dx_acc, xt, dw_tx, dw_rx, sum_tx,
    in_send, in_recv, lam_send, lam_recv, x_send, x_recv, w_sem,
    st_send, st_recv, out_send, out_recv, dk_send, dk_fwd, dk_recv,
    dx_send, dx_recv, rs_send, rs_recv, ag_send, ag_recv,
):
    s = lax.axis_index("sp")
    d = lax.axis_index("dp")
    gz = s // GROUP
    me = s % GROUP
    head = (me + 4 * gz) % GROUP
    base = GROUP * gz
    partner = GROUP * (1 - gz) + (head + 4 * (1 - gz)) % GROUP
    xi, core = d // 2, d % 2
    sibling = 2 * xi + 1 - core

    def col(i, width):
        return pl.ds(pl.multiple_of(i * width, width), width)

    def remote(src, dst, ssem, rsem, to):
        return pltpu.make_async_remote_copy(
            src_ref=src, dst_ref=dst, send_sem=ssem, recv_sem=rsem,
            device_id=to, device_id_type=MESH,
        )

    def arrived(dst, sem):
        pltpu.make_async_copy(dst, dst, sem).wait()

    barrier = pltpu.get_barrier_semaphore()

    @pl.loop(1, SP)
    def _(i):
        pl.semaphore_signal(barrier, inc=1, device_id=((s + i) % SP, d), device_id_type=MESH)

    @pl.loop(1, DPN)
    def _(i):
        pl.semaphore_signal(barrier, inc=1, device_id=(s, (d + i) % DPN), device_id_type=MESH)

    pl.semaphore_wait(barrier, SP + DPN - 2)

    lam_to = [s // 2, GROUP + (s // 2 + 4) % GROUP]
    for half in range(2):
        src = lam_ref.at[pl.ds(8 * half, 8), :]

        @pl.when(lam_to[half] == s)
        def _():
            pltpu.make_async_copy(src, rlam.at[s % 2], lam_recv.at[s % 2]).start()

        @pl.when(lam_to[half] != s)
        def _():
            remote(src, rlam.at[s % 2], lam_send.at[half], lam_recv.at[s % 2], (lam_to[half], d)).start()

    pairs = ((g_ref, rg, DV), (q_ref, rq, DK), (v_ref, rv, DV), (k_ref, rk, DK))
    for n, (src, dst, width) in enumerate(pairs):
        pltpu.make_async_copy(src.at[:, col(head, width)], dst.at[me], in_recv.at[n, me]).start()

    for n, (src, dst, width) in enumerate(pairs):

        @pl.loop(1, GROUP)
        def _(i):
            to = (me + i) % GROUP
            its_head = (to + 4 * gz) % GROUP
            remote(
                src.at[:, col(its_head, width)], dst.at[me],
                in_send.at[n, to], in_recv.at[n, me], (base + to, d),
            ).start()

    pltpu.make_async_copy(x_ref.at[:, col(d, 256)], x_all.at[d], x_recv.at[d]).start()

    @pl.loop(1, DPN)
    def _(i):
        to = (d + i) % DPN
        remote(x_ref.at[:, col(to, 256)], x_all.at[d], x_send.at[to], x_recv.at[d], (s, to)).start()

    w_copy = pltpu.make_async_copy(w_ref, w_all, w_sem)
    w_copy.start()

    for r in range(2):
        arrived(rlam.at[r], lam_recv.at[r])
    row = lax.broadcasted_iota(jnp.int32, (BLOCK, BLOCK), 0)
    column = lax.broadcasted_iota(jnp.int32, (BLOCK, BLOCK), 1)
    ones = jnp.ones((BLOCK, BLOCK), F32)
    hi = lax.Precision.HIGHEST

    @pl.loop(0, GROUP)
    def _(b):
        kept = []
        for r in range(2):
            lam = jnp.broadcast_to(rlam[r, pl.ds(b, 1), :], (BLOCK, BLOCK))
            seen = column <= row if r == 0 else column >= row
            c = dot(jnp.where(seen, lam, 0.0), ones, 1, 0, hi)
            kept.append(c - c.T)
            end = c[BLOCK - 1 : BLOCK, :] if r == 0 else c[0:1, :]
            qs[r, b] = jnp.exp(c) * 0.0625
            ks[r, b] = jnp.exp(end - c)
            ee[r, b] = jnp.broadcast_to(end, (8, 128))
        wgt[b] = jnp.exp(jnp.where(column <= row, kept[0], kept[1])) * 0.0625

    for r in range(2):
        up = jnp.zeros((8, 128), F32)
        down = jnp.zeros((8, 128), F32)
        for b in range(GROUP):
            tails[r, 1, b] = jnp.exp(down)
            down = down + ee[r, b]
            tails[r, 0, GROUP - 1 - b] = jnp.exp(up)
            up = up + ee[r, GROUP - 1 - b]
        for b in range(GROUP):
            ee[r, b] = jnp.exp(ee[r, b])

    def order(i, way):
        return i + way * (GROUP - 1 - 2 * i)

    def send_state(st, n):
        st_tx[n] = st[...].astype(BF16)
        remote(st_tx.at[n], st_rx.at[n], st_send.at[n], st_recv.at[n], (partner, d)).start()

    def scaled(block, scale):
        return (block.astype(F32) * lanes(scale, DK)).astype(BF16)

    st[...] = jnp.zeros_like(st)

    @pl.loop(0, GROUP)
    def _(i):
        b = (me + GROUP - i) % GROUP
        for n in (0, 1):
            arrived(pairs[n][1].at[b], in_recv.at[n, b])
        st[...] += dot(scaled(rq[b], qs[1 - gz, b] * tails[1 - gz, gz, b][0:1, :]), rg[b], 0, 0)

    send_state(st, 0)

    def g_chain(way):
        r = 1 - way

        @pl.loop(0, GROUP)
        def _(i):
            b = order(i, way)
            g_all[r, b] = st[...].astype(BF16)
            st[...] = st[...] * lanes(ee[r, b][0:1, :], DV) + dot(scaled(rq[b], qs[r, b]), rg[b], 0, 0)

    st[...] = jnp.zeros_like(st)
    g_chain(gz)
    arrived(st_rx.at[0], st_recv.at[0])
    st[...] = st_rx[0].astype(F32)
    g_chain(1 - gz)

    homes = (
        (out_k, dk_all.at[d], DK),
        (out_v, dv_ref, DV),
        (out_q, dq_ref, DK),
    )

    def send_home(b, n):
        src, dst, width = homes[n]

        @pl.when(b == me)
        def _():
            pltpu.make_async_copy(src.at[b], dst.at[:, col(head, width)], out_recv.at[n, head]).start()

        @pl.when(b != me)
        def _():
            remote(
                src.at[b], dst.at[:, col(head, width)],
                out_send.at[n, b], out_recv.at[n, head], (base + b, d),
            ).start()

    st[...] = jnp.zeros_like(st)

    @pl.loop(0, GROUP)
    def _(i):
        b = (me + GROUP - i) % GROUP
        for n in (2, 3):
            arrived(pairs[n][1].at[b], in_recv.at[n, b])
        v = rv[b]
        gs = (dot(rg[b], v, 1, 1) * wgt[b]).astype(BF16)
        gs_all[b] = gs
        dk = dot(gs, rq[b], 0, 0)
        for r in range(2):
            dk += dot(v, g_all[r, b], 1, 1) * lanes(ks[r, b], DK)
        out_k[b] = dk.astype(BF16)
        send_home(b, 0)
        st[...] += dot(scaled(rk[b], ks[gz, b] * tails[gz, gz, b][0:1, :]), v, 0, 0)

    send_state(st, 1)

    @pl.loop(0, GROUP)
    def _(i):
        b = (me + GROUP - i) % GROUP
        k = rk[b]
        dv = dot((dot(rq[b], k, 1, 1) * wgt[b]).astype(BF16), rg[b], 0, 0)
        for r in range(2):
            dv += dot(scaled(k, ks[r, b]), g_all[r, b], 1, 0)
        out_v[b] = dv.astype(BF16)
        send_home(b, 1)

    def m_step(b, r):
        dq = dot(rg[b], st[...].astype(BF16), 1, 1) * lanes(qs[r, b], DK)
        st[...] = st[...] * lanes(ee[r, b][0:1, :], DV) + dot(scaled(rk[b], ks[r, b]), rv[b], 0, 0)
        return dq

    st[...] = jnp.zeros_like(st)

    @pl.loop(0, GROUP)
    def _(i):
        b = order(i, gz)
        acc_q[b] = m_step(b, gz) + dot(gs_all[b], rk[b], 1, 0)

    @pl.loop(0, GROUP)
    def _(h):
        arrived(out_k.at[h], out_recv.at[0, h])

    def piece(j, c):
        return dk_all.at[j, :, col(c, CHUNK)]

    for c in range(CHUNKS):
        own = piece(d, c)
        remote(own, own, dk_send.at[0, c], dk_recv.at[d, c], (s, sibling)).start()
        for t in (1, 3, 2):
            remote(own, own, dk_send.at[t, c], dk_recv.at[d, c], (s, 2 * ((xi + t) % 4) + core)).start()

    arrived(st_rx.at[1], st_recv.at[1])
    st[...] = st_rx[1].astype(F32)

    @pl.loop(0, GROUP)
    def _(i):
        b = order(i, 1 - gz)
        out_q[b] = (acc_q[b] + m_step(b, 1 - gz)).astype(BF16)
        send_home(b, 2)

    @pl.loop(0, DPN)
    def _(j):
        arrived(x_all.at[j], x_recv.at[j])
        xt[:, col(j, BLOCK)] = x_all[j].T

    w_copy.wait()
    dx_acc[...] = jnp.zeros_like(dx_acc)

    def sum_chunk(c):
        arrived(dw_rx.at[c], rs_recv.at[c])
        sum_tx[c] = jnp.sum(dw_rx[c].astype(F32), axis=0).astype(BF16)
        place = dw_ref.at[pl.ds(pl.multiple_of(16 * s, 16), 16), col(c, CHUNK)]
        pltpu.make_async_copy(sum_tx.at[c], place, ag_recv.at[c]).start()

        @pl.loop(1, SP)
        def _(i):
            remote(sum_tx.at[c], place, ag_send.at[c], ag_recv.at[c], ((s + i) % SP, d)).start()

    @pl.loop(0, CHUNKS)
    def _(c):
        arrived(piece(sibling, c), dk_recv.at[sibling, c])
        for n, t in enumerate((1, 3, 2)):
            near = 2 * ((xi + t) % 4) + core
            arrived(piece(near, c), dk_recv.at[near, c])
            remote(piece(near, c), piece(near, c), dk_fwd.at[n, c], dk_recv.at[near, c], (s, sibling)).start()
        for t in (1, 3, 2):
            far = 2 * ((xi + t) % 4) + 1 - core
            arrived(piece(far, c), dk_recv.at[far, c])
        part = dk_all[:, :, col(c, CHUNK)].reshape(DPN * BLOCK, CHUNK)
        dw_tx[c] = dot(xt[...], part, 1, 0).astype(BF16)
        pltpu.make_async_copy(
            dw_tx.at[c, pl.ds(pl.multiple_of(16 * s, 16), 16), :], dw_rx.at[c, s], rs_recv.at[c]
        ).start()

        @pl.loop(1, SP)
        def _(i):
            to = (s + i) % SP
            remote(
                dw_tx.at[c, pl.ds(pl.multiple_of(16 * to, 16), 16), :], dw_rx.at[c, s],
                rs_send.at[c], rs_recv.at[c], (to, d),
            ).start()

        dx_acc[...] += dot(part, w_all[:, col(c, CHUNK)], 1, 1)

        @pl.when(c > 0)
        def _():
            sum_chunk(c - 1)

    for j in range(DPN):
        dx_st[j] = dx_acc[BLOCK * j : BLOCK * (j + 1), :].astype(BF16)
    columns = dx_ref.at[:, col(d, 256)]
    pltpu.make_async_copy(dx_st.at[d], columns, dx_recv.at[d]).start()

    @pl.loop(1, DPN)
    def _(i):
        to = (d + i) % DPN
        remote(dx_st.at[to], columns, dx_send.at[to], dx_recv.at[d], (s, to)).start()

    sum_chunk(CHUNKS - 1)

    @pl.loop(0, GROUP)
    def _(h):
        arrived(out_v.at[h], out_recv.at[1, h])
        arrived(out_q.at[h], out_recv.at[2, h])

    @pl.loop(0, DPN)
    def _(j):
        arrived(dx_st.at[j], dx_recv.at[j])

    for half in range(2):

        @pl.when(lam_to[half] != s)
        def _():
            arrived(rlam.at[half], lam_send.at[half])

    @pl.loop(1, GROUP)
    def _(i):
        to = (me + i) % GROUP
        for n, (_, dst, _) in enumerate(pairs):
            arrived(dst.at[to], in_send.at[n, to])
        for n, (src, _, _) in enumerate(homes):
            arrived(src.at[to], out_send.at[n, to])

    @pl.loop(1, DPN)
    def _(i):
        to = (d + i) % DPN
        arrived(x_all.at[to], x_send.at[to])
        arrived(dx_st.at[to], dx_send.at[to])

    for n in range(2):
        arrived(st_tx.at[n], st_send.at[n])

    @pl.loop(0, CHUNKS)
    def _(c):
        own = piece(d, c)
        for t in range(4):
            arrived(own, dk_send.at[t, c])
        for t in range(3):
            arrived(own, dk_fwd.at[t, c])
        most = dw_rx.at[c, pl.ds(0, SP - 1)]
        arrived(most, rs_send.at[c])
        arrived(most, ag_send.at[c])
        arrived(dw_ref.at[:, col(c, CHUNK)], ag_recv.at[c])


def step(x, q, k, v, g, lam, w):
    vmem = pl.BlockSpec(memory_space=pltpu.VMEM)
    hbm = pl.BlockSpec(memory_space=pl.ANY)
    dma = pltpu.SemaphoreType.DMA
    v_ = pltpu.VMEM
    dq, dv, dx, dw = pl.pallas_call(
        kernel,
        out_shape=(
            jax.ShapeDtypeStruct((BLOCK, 2048), BF16),
            jax.ShapeDtypeStruct((BLOCK, 4096), BF16),
            jax.ShapeDtypeStruct((BLOCK, 2048), BF16),
            jax.ShapeDtypeStruct((256, 2048), BF16),
        ),
        in_specs=[hbm, vmem, vmem, vmem, vmem, vmem, hbm],
        out_specs=(vmem,) * 4,
        scratch_shapes=[
            v_((8, BLOCK, DK), BF16), v_((8, BLOCK, DK), BF16),
            v_((8, BLOCK, DV), BF16), v_((8, BLOCK, DV), BF16),
            v_((2, 8, 128), F32), v_((256, 2048), BF16), v_((8, BLOCK, 256), BF16),
            v_((2, 8, BLOCK, 128), F32), v_((2, 8, BLOCK, 128), F32),
            v_((2, 8, 8, 128), F32), v_((2, 2, 8, 8, 128), F32), v_((8, BLOCK, 128), F32),
            v_((8, BLOCK, DK), F32), v_((8, BLOCK, BLOCK), BF16), v_((2, 8, DK, DV), BF16),
            v_((DK, DV), F32), v_((2, DK, DV), BF16), v_((2, DK, DV), BF16),
            v_((8, BLOCK, DK), BF16), v_((8, BLOCK, DK), BF16), v_((8, BLOCK, DV), BF16),
            v_((8, BLOCK, D), BF16), v_((8, BLOCK, 256), BF16), v_((8 * BLOCK, 256), F32),
            v_((256, 8 * BLOCK), BF16), v_((CHUNKS, 256, CHUNK), BF16),
            v_((CHUNKS, 16, 16, CHUNK), BF16), v_((CHUNKS, 16, CHUNK), BF16),
            dma((4, 8)), dma((4, 8)), dma((2,)), dma((2,)), dma((8,)), dma((8,)), dma,
            dma((2,)), dma((2,)), dma((3, 8)), dma((3, 8)),
            dma((4, CHUNKS)), dma((3, CHUNKS)), dma((8, CHUNKS)), dma((8,)), dma((8,)),
            dma((CHUNKS,)), dma((CHUNKS,)), dma((CHUNKS,)), dma((CHUNKS,)),
        ],
        compiler_params=pltpu.CompilerParams(
            collective_id=0, has_side_effects=True, vmem_limit_bytes=60 * 1024 * 1024
        ),
    )(x[0], q[0], k[0], v[0], g[0], lam[0].reshape(16, 128), w)
    return dq[None], dv[None], dx[None], dw.astype(F32)


def solution(mesh):
    tokens = P("dp", "sp", None)
    return jax.shard_map(
        step,
        mesh=mesh,
        in_specs=(tokens,) * 6 + (P("dp", None),),
        out_specs=(tokens, tokens, tokens, P("dp", None)),
        check_vma=False,
    )
```

```python
import functools

import jax
import jax.numpy as jnp
from jax import lax
from jax.experimental import pallas as pl
from jax.experimental.pallas import tpu as pltpu
from jax.sharding import PartitionSpec as P

F32 = jnp.float32
BF16 = jnp.bfloat16
SP, DPN = 16, 8
GROUP = 8
DK, DV, D = 256, 512, 2048
BLOCK = 128
CHUNKS = 4
CHUNK = D // CHUNKS
MESH = pl.DeviceIdType.MESH


def dot(a, b, ca, cb, precision=None):
    return lax.dot_general(
        a, b, (((ca,), (cb,)), ((), ())), preferred_element_type=F32, precision=precision
    )


def lanes(scale, width):
    return jnp.concatenate([scale] * (width // 128), axis=1)


def kernel(
    x_ref, q_ref, k_ref, v_ref, g_ref, lam_ref, w_ref,
    dq_ref, dv_ref, dx_ref, dw_ref,
    rq, rk, rv, rg, rlam, w_all, x_all,
    qs, ks, ee, tails, wgt,
    acc_q, gs_all, g_all, st, st_tx, st_rx, out_q, out_k, out_v,
    dk_all, dx_st, dx_acc, xt, dw_tx, dw_rx, sum_tx, dw_sum,
    in_send, in_recv, lam_send, lam_recv, x_send, x_recv, w_sem,
    st_send, st_recv, out_send, out_recv, dk_send, dk_fwd, dk_recv,
    dx_send, dx_recv, rs_send, rs_recv, ag_send, ag_recv,
):
    s = lax.axis_index("sp")
    d = lax.axis_index("dp")
    gz = s // GROUP
    me = s % GROUP
    head = (me + 4 * gz) % GROUP
    base = GROUP * gz
    partner = GROUP * (1 - gz) + (head + 4 * (1 - gz)) % GROUP
    xi, core = d // 2, d % 2
    sibling = 2 * xi + 1 - core

    def col(i, width):
        return pl.ds(pl.multiple_of(i * width, width), width)

    def remote(src, dst, ssem, rsem, to):
        return pltpu.make_async_remote_copy(
            src_ref=src, dst_ref=dst, send_sem=ssem, recv_sem=rsem,
            device_id=to, device_id_type=MESH,
        )

    def arrived(dst, sem):
        pltpu.make_async_copy(dst, dst, sem).wait()

    barrier = pltpu.get_barrier_semaphore()

    @pl.loop(1, SP)
    def _(i):
        pl.semaphore_signal(barrier, inc=1, device_id=((s + i) % SP, d), device_id_type=MESH)

    @pl.loop(1, DPN)
    def _(i):
        pl.semaphore_signal(barrier, inc=1, device_id=(s, (d + i) % DPN), device_id_type=MESH)

    pl.semaphore_wait(barrier, SP + DPN - 2)

    lam_to = [s // 2, GROUP + (s // 2 + 4) % GROUP]
    for half in range(2):
        src = lam_ref.at[pl.ds(8 * half, 8), :]

        @pl.when(lam_to[half] == s)
        def _():
            pltpu.make_async_copy(src, rlam.at[s % 2], lam_recv.at[s % 2]).start()

        @pl.when(lam_to[half] != s)
        def _():
            remote(src, rlam.at[s % 2], lam_send.at[half], lam_recv.at[s % 2], (lam_to[half], d)).start()

    pairs = ((g_ref, rg, DV), (q_ref, rq, DK), (v_ref, rv, DV), (k_ref, rk, DK))
    for n, (src, dst, width) in enumerate(pairs):
        pltpu.make_async_copy(src.at[:, col(head, width)], dst.at[me], in_recv.at[n, me]).start()

    pltpu.make_async_copy(x_ref.at[:, col(d, 256)], x_all.at[d], x_recv.at[d]).start()

    for n, (src, dst, width) in enumerate(pairs):

        @pl.loop(1, GROUP)
        def _(i):
            to = (me + i) % GROUP
            its_head = (to + 4 * gz) % GROUP
            remote(
                src.at[:, col(its_head, width)], dst.at[me],
                in_send.at[n, to], in_recv.at[n, me], (base + to, d),
            ).start()
            if n == 1:
                its = (d + i) % DPN
                remote(x_ref.at[:, col(its, 256)], x_all.at[d], x_send.at[its], x_recv.at[d], (s, its)).start()

    w_copy = pltpu.make_async_copy(w_ref, w_all, w_sem)
    w_copy.start()

    for r in range(2):
        arrived(rlam.at[r], lam_recv.at[r])
    row = lax.broadcasted_iota(jnp.int32, (BLOCK, BLOCK), 0)
    column = lax.broadcasted_iota(jnp.int32, (BLOCK, BLOCK), 1)
    ones = jnp.ones((BLOCK, BLOCK), F32)
    hi = lax.Precision.HIGHEST

    @pl.loop(0, GROUP)
    def _(b):
        kept = []
        for r in range(2):
            lam = jnp.broadcast_to(rlam[r, pl.ds(b, 1), :], (BLOCK, BLOCK))
            seen = column <= row if r == 0 else column >= row
            c = dot(jnp.where(seen, lam, 0.0), ones, 1, 0, hi)
            kept.append(c - c.T)
            end = c[BLOCK - 1 : BLOCK, :] if r == 0 else c[0:1, :]
            qs[r, b] = jnp.exp(c) * 0.0625
            ks[r, b] = jnp.exp(end - c)
            ee[r, b] = jnp.broadcast_to(end, (8, 128))
        wgt[b] = jnp.exp(jnp.where(column <= row, kept[0], kept[1])) * 0.0625

    for r in range(2):
        up = jnp.zeros((8, 128), F32)
        down = jnp.zeros((8, 128), F32)
        for b in range(GROUP):
            tails[r, 1, b] = jnp.exp(down)
            down = down + ee[r, b]
            tails[r, 0, GROUP - 1 - b] = jnp.exp(up)
            up = up + ee[r, GROUP - 1 - b]
        for b in range(GROUP):
            ee[r, b] = jnp.exp(ee[r, b])

    def order(i, way):
        return i + way * (GROUP - 1 - 2 * i)

    def send_state(st, n):
        st_tx[n] = st[...].astype(BF16)
        remote(st_tx.at[n], st_rx.at[n], st_send.at[n], st_recv.at[n], (partner, d)).start()

    def scaled(block, scale):
        return (block.astype(F32) * lanes(scale, DK)).astype(BF16)

    st[...] = jnp.zeros_like(st)

    @pl.loop(0, GROUP)
    def _(i):
        b = (me + GROUP - i) % GROUP
        for n in (0, 1):
            arrived(pairs[n][1].at[b], in_recv.at[n, b])
        st[...] += dot(scaled(rq[b], qs[1 - gz, b] * tails[1 - gz, gz, b][0:1, :]), rg[b], 0, 0)

    send_state(st, 0)

    def g_chain(way):
        r = 1 - way

        @pl.loop(0, GROUP)
        def _(i):
            b = order(i, way)
            g_all[r, b] = st[...].astype(BF16)
            st[...] = st[...] * lanes(ee[r, b][0:1, :], DV) + dot(scaled(rq[b], qs[r, b]), rg[b], 0, 0)

    st[...] = jnp.zeros_like(st)
    g_chain(gz)
    arrived(st_rx.at[0], st_recv.at[0])
    st[...] = st_rx[0].astype(F32)
    g_chain(1 - gz)

    homes = (
        (out_k, dk_all.at[d], DK),
        (out_v, dv_ref, DV),
        (out_q, dq_ref, DK),
    )

    def send_home(b, n):
        src, dst, width = homes[n]

        @pl.when(b == me)
        def _():
            pltpu.make_async_copy(src.at[b], dst.at[:, col(head, width)], out_recv.at[n, head]).start()

        @pl.when(b != me)
        def _():
            remote(
                src.at[b], dst.at[:, col(head, width)],
                out_send.at[n, b], out_recv.at[n, head], (base + b, d),
            ).start()

    @pl.loop(0, GROUP)
    def _(i):
        b = (me + GROUP - i) % GROUP
        arrived(rv.at[b], in_recv.at[2, b])
        v = rv[b]
        gs = (dot(rg[b], v, 1, 1) * wgt[b]).astype(BF16)
        gs_all[b] = gs
        dk = dot(gs, rq[b], 0, 0)
        for r in range(2):
            dk += dot(v, g_all[r, b], 1, 1) * lanes(ks[r, b], DK)
        out_k[b] = dk.astype(BF16)
        send_home(b, 0)

    st[...] = jnp.zeros_like(st)

    @pl.loop(0, GROUP)
    def _(i):
        b = (me + GROUP - i) % GROUP
        arrived(rk.at[b], in_recv.at[3, b])
        st[...] += dot(scaled(rk[b], ks[gz, b] * tails[gz, gz, b][0:1, :]), rv[b], 0, 0)

    send_state(st, 1)

    def piece(j, c):
        return dk_all.at[j, :, col(c, CHUNK)]

    left = 2 * ((xi + 3) % 4) + core
    right = 2 * ((xi + 1) % 4) + core
    across = 2 * ((xi + 2) % 4) + core

    def pass_on(j, c, sem, to):
        remote(piece(j, c), piece(j, c), sem, dk_recv.at[j, c], (s, to)).start()

    @pl.loop(0, GROUP)
    def _(i):
        b = (me + GROUP - i) % GROUP
        k = rk[b]
        dv = dot((dot(rq[b], k, 1, 1) * wgt[b]).astype(BF16), rg[b], 0, 0)
        for r in range(2):
            dv += dot(scaled(k, ks[r, b]), g_all[r, b], 1, 0)
        out_v[b] = dv.astype(BF16)
        send_home(b, 1)

        c = i // 2

        @pl.when(i % 2 == 0)
        def _():
            for h in range(CHUNK // DK):
                arrived(out_k.at[0], out_recv.at[0, c * (CHUNK // DK) + h])
            pass_on(d, c, dk_send.at[0, c], left)
            pass_on(d, c, dk_send.at[1, c], right)

        @pl.when(i % 2 == 1)
        def _():
            pass_on(d, c, dk_send.at[2, c], across)
            pass_on(d, c, dk_send.at[3, c], sibling)

    def m_step(b, r):
        dq = dot(rg[b], st[...].astype(BF16), 1, 1) * lanes(qs[r, b], DK)
        st[...] = st[...] * lanes(ee[r, b][0:1, :], DV) + dot(scaled(rk[b], ks[r, b]), rv[b], 0, 0)
        return dq

    st[...] = jnp.zeros_like(st)

    @pl.loop(0, GROUP)
    def _(i):
        b = order(i, gz)
        acc_q[b] = m_step(b, gz) + dot(gs_all[b], rk[b], 1, 0)

    @pl.loop(0, DPN)
    def _(j):
        arrived(x_all.at[j], x_recv.at[j])
        xt[:, col(j, BLOCK)] = x_all[j].T

    w_copy.wait()
    dx_acc[...] = jnp.zeros_like(dx_acc)

    arrived(st_rx.at[1], st_recv.at[1])
    st[...] = st_rx[1].astype(F32)

    @pl.loop(0, GROUP)
    def _(i):
        b = order(i, 1 - gz)
        out_q[b] = (acc_q[b] + m_step(b, 1 - gz)).astype(BF16)
        send_home(b, 2)

    def sum_chunk(c):
        arrived(dw_rx.at[c], rs_recv.at[c])
        sum_tx[c] = jnp.sum(dw_rx[c].astype(F32), axis=0).astype(BF16)
        place = dw_sum.at[pl.ds(pl.multiple_of(16 * s, 16), 16), col(c, CHUNK)]
        pltpu.make_async_copy(sum_tx.at[c], place, ag_recv.at[c]).start()

        @pl.loop(1, SP)
        def _(i):
            remote(sum_tx.at[c], place, ag_send.at[c], ag_recv.at[c], ((s + i) % SP, d)).start()

    @pl.loop(0, CHUNKS)
    def _(c):
        for n, j in enumerate((left, right, across)):
            arrived(piece(j, c), dk_recv.at[j, c])
            pass_on(j, c, dk_fwd.at[n, c], sibling)
        for j in range(4):
            far = 2 * ((xi + j) % 4) + 1 - core
            arrived(piece(far, c), dk_recv.at[far, c])
        part = dk_all[:, :, col(c, CHUNK)].reshape(DPN * BLOCK, CHUNK)
        dw_tx[c] = dot(xt[...], part, 1, 0).astype(BF16)
        pltpu.make_async_copy(
            dw_tx.at[c, pl.ds(pl.multiple_of(16 * s, 16), 16), :], dw_rx.at[c, s], rs_recv.at[c]
        ).start()

        @pl.loop(1, SP)
        def _(i):
            to = (s + i) % SP
            remote(
                dw_tx.at[c, pl.ds(pl.multiple_of(16 * to, 16), 16), :], dw_rx.at[c, s],
                rs_send.at[c], rs_recv.at[c], (to, d),
            ).start()

        dx_acc[...] += dot(part, w_all[:, col(c, CHUNK)], 1, 1)

        @pl.when(c > 0)
        def _():
            sum_chunk(c - 1)

    for j in range(DPN):
        dx_st[j] = dx_acc[BLOCK * j : BLOCK * (j + 1), :].astype(BF16)
    columns = dx_ref.at[:, col(d, 256)]
    pltpu.make_async_copy(dx_st.at[d], columns, dx_recv.at[d]).start()

    @pl.loop(1, DPN)
    def _(i):
        to = (d + i) % DPN
        remote(dx_st.at[to], columns, dx_send.at[to], dx_recv.at[d], (s, to)).start()

    sum_chunk(CHUNKS - 1)

    @pl.loop(0, GROUP)
    def _(h):
        arrived(out_v.at[h], out_recv.at[1, h])
        arrived(out_q.at[h], out_recv.at[2, h])

    @pl.loop(0, DPN)
    def _(j):
        arrived(dx_st.at[j], dx_recv.at[j])

    for half in range(2):

        @pl.when(lam_to[half] != s)
        def _():
            arrived(rlam.at[half], lam_send.at[half])

    @pl.loop(1, GROUP)
    def _(i):
        to = (me + i) % GROUP
        for n, (_, dst, _) in enumerate(pairs):
            arrived(dst.at[to], in_send.at[n, to])
        for n, (src, _, _) in enumerate(homes):
            arrived(src.at[to], out_send.at[n, to])

    @pl.loop(1, DPN)
    def _(i):
        to = (d + i) % DPN
        arrived(x_all.at[to], x_send.at[to])
        arrived(dx_st.at[to], dx_send.at[to])

    for n in range(2):
        arrived(st_tx.at[n], st_send.at[n])

    @pl.loop(0, CHUNKS)
    def _(c):
        own = piece(d, c)
        for t in range(4):
            arrived(own, dk_send.at[t, c])
        for t in range(3):
            arrived(own, dk_fwd.at[t, c])
        most = dw_rx.at[c, pl.ds(0, SP - 1)]
        arrived(most, rs_send.at[c])
        arrived(most, ag_send.at[c])
        arrived(dw_sum.at[:, col(c, CHUNK)], ag_recv.at[c])
        dw_ref[:, col(c, CHUNK)] = dw_sum[:, col(c, CHUNK)].astype(F32)


def write_out(*refs):
    sems = refs[-1]
    copies = [pltpu.make_async_copy(refs[n], refs[n + 4], sems.at[n]) for n in range(4)]
    for copy in copies:
        copy.start()
    for copy in copies:
        copy.wait()


def step(x, q, k, v, g, lam, w):
    vmem = pl.BlockSpec(memory_space=pltpu.VMEM)
    hbm = pl.BlockSpec(memory_space=pl.ANY)
    dma = pltpu.SemaphoreType.DMA
    v_ = pltpu.VMEM
    results = pl.pallas_call(
        kernel,
        out_shape=(
            v_((BLOCK, 2048), BF16), v_((BLOCK, 4096), BF16), v_((BLOCK, 2048), BF16), v_((256, 2048), F32)
        ),
        in_specs=[hbm, hbm, hbm, hbm, hbm, vmem, hbm],
        out_specs=(vmem,) * 4,
        scratch_shapes=[
            v_((8, BLOCK, DK), BF16), v_((8, BLOCK, DK), BF16),
            v_((8, BLOCK, DV), BF16), v_((8, BLOCK, DV), BF16),
            v_((2, 8, 128), F32), v_((256, 2048), BF16), v_((8, BLOCK, 256), BF16),
            v_((2, 8, BLOCK, 128), F32), v_((2, 8, BLOCK, 128), F32),
            v_((2, 8, 8, 128), F32), v_((2, 2, 8, 8, 128), F32), v_((8, BLOCK, 128), F32),
            v_((8, BLOCK, DK), F32), v_((8, BLOCK, BLOCK), BF16), v_((2, 8, DK, DV), BF16),
            v_((DK, DV), F32), v_((2, DK, DV), BF16), v_((2, DK, DV), BF16),
            v_((8, BLOCK, DK), BF16), v_((8, BLOCK, DK), BF16), v_((8, BLOCK, DV), BF16),
            v_((8, BLOCK, D), BF16), v_((8, BLOCK, 256), BF16), v_((8 * BLOCK, 256), F32),
            v_((256, 8 * BLOCK), BF16), v_((CHUNKS, 256, CHUNK), BF16),
            v_((CHUNKS, 16, 16, CHUNK), BF16), v_((CHUNKS, 16, CHUNK), BF16), v_((256, D), BF16),
            dma((4, 8)), dma((4, 8)), dma((2,)), dma((2,)), dma((8,)), dma((8,)), dma,
            dma((2,)), dma((2,)), dma((3, 8)), dma((3, 8)),
            dma((4, CHUNKS)), dma((3, CHUNKS)), dma((8, CHUNKS)), dma((8,)), dma((8,)),
            dma((CHUNKS,)), dma((CHUNKS,)), dma((CHUNKS,)), dma((CHUNKS,)),
        ],
        compiler_params=pltpu.CompilerParams(
            collective_id=0, has_side_effects=True, vmem_limit_bytes=58 * 1024 * 1024
        ),
    )(x[0], q[0], k[0], v[0], g[0], lam[0].reshape(16, 128), w)
    dq, dv, dx, dw = pl.pallas_call(
        write_out,
        out_shape=tuple(pltpu.HBM(a.shape, a.dtype) for a in results),
        in_specs=[hbm] * 4,
        out_specs=(hbm,) * 4,
        scratch_shapes=[dma((4,))],
        compiler_params=pltpu.CompilerParams(vmem_limit_bytes=20 * 1024 * 1024),
    )(*results)
    return dq[None], dv[None], dx[None], dw


def solution(mesh):
    tokens = P("dp", "sp", None)
    return jax.shard_map(
        step,
        mesh=mesh,
        in_specs=(tokens,) * 6 + (P("dp", None),),
        out_specs=(tokens, tokens, tokens, P("dp", None)),
        check_vma=False,
    )
```

```python
import functools

import jax
import jax.numpy as jnp
from jax import lax
from jax.experimental import pallas as pl
from jax.experimental.pallas import tpu as pltpu
from jax.sharding import PartitionSpec as P

F32 = jnp.float32
BF16 = jnp.bfloat16
SP, DPN = 16, 8
GROUP = 8
DK, DV, D = 256, 512, 2048
BLOCK = 128
CHUNKS = 4
CHUNK = D // CHUNKS
LAST = CHUNKS - 1
MESH = pl.DeviceIdType.MESH


def dot(a, b, ca, cb, precision=None):
    return lax.dot_general(
        a, b, (((ca,), (cb,)), ((), ())), preferred_element_type=F32, precision=precision
    )


def lanes(scale, width):
    return jnp.concatenate([scale] * (width // 128), axis=1)


def kernel(
    x_ref, q_ref, k_ref, v_ref, g_ref, lam_ref, w_ref,
    dq_ref, dv_ref, dx_ref, dw_ref,
    rq, rk, rv, rg, rlam, w_all, x_all,
    qs, ks, ee, tails, wgt,
    acc_q, gs_all, g_all, st, st_tx, st_rx, out_q, out_k, out_v,
    dk_all, dx_st, dx_acc, xt, dw_tx, rx_one, tx_two, rx_two, dw_rx, sum_tx, dw_sum,
    in_send, in_recv, lam_send, lam_recv, x_send, x_recv, w_sem,
    st_send, st_recv, out_send, out_recv, dk_send, dk_fwd, dk_recv,
    dx_send, dx_recv, sum_send, sum_recv, last_send, last_recv,
):
    s = lax.axis_index("sp")
    d = lax.axis_index("dp")
    gz = s // GROUP
    me = s % GROUP
    head = (me + 4 * gz) % GROUP
    base = GROUP * gz
    partner = GROUP * (1 - gz) + (head + 4 * (1 - gz)) % GROUP
    xi, core = d // 2, d % 2
    sibling = 2 * xi + 1 - core

    def col(i, width):
        return pl.ds(pl.multiple_of(i * width, width), width)

    def remote(src, dst, ssem, rsem, to):
        return pltpu.make_async_remote_copy(
            src_ref=src, dst_ref=dst, send_sem=ssem, recv_sem=rsem,
            device_id=to, device_id_type=MESH,
        )

    def arrived(dst, sem):
        pltpu.make_async_copy(dst, dst, sem).wait()

    barrier = pltpu.get_barrier_semaphore()

    @pl.loop(1, SP)
    def _(i):
        pl.semaphore_signal(barrier, inc=1, device_id=((s + i) % SP, d), device_id_type=MESH)

    @pl.loop(1, DPN)
    def _(i):
        pl.semaphore_signal(barrier, inc=1, device_id=(s, (d + i) % DPN), device_id_type=MESH)

    pl.semaphore_wait(barrier, SP + DPN - 2)

    lam_to = [s // 2, GROUP + (s // 2 + 4) % GROUP]
    for half in range(2):
        src = lam_ref.at[pl.ds(8 * half, 8), :]

        @pl.when(lam_to[half] == s)
        def _():
            pltpu.make_async_copy(src, rlam.at[s % 2], lam_recv.at[s % 2]).start()

        @pl.when(lam_to[half] != s)
        def _():
            remote(src, rlam.at[s % 2], lam_send.at[half], lam_recv.at[s % 2], (lam_to[half], d)).start()

    pairs = ((g_ref, rg, DV), (q_ref, rq, DK), (v_ref, rv, DV), (k_ref, rk, DK))
    for n, (src, dst, width) in enumerate(pairs):
        pltpu.make_async_copy(src.at[:, col(head, width)], dst.at[me], in_recv.at[n, me]).start()

    row_here, y_here = me // 4, me % 4
    near_y = (y_here + 1 - 2 * (y_here % 2), 3 - y_here)
    farthest_first = [4 * (1 - row_here) + (y_here + 2) % 4, 4 * row_here + (y_here + 2) % 4]
    farthest_first += [4 * (1 - row_here) + y for y in near_y] + [4 * (1 - row_here) + y_here]
    farthest_first += [4 * row_here + y for y in near_y]

    def nth(i):
        b = me
        for n, to in enumerate(farthest_first):
            b = jnp.where(i == n, to, b)
        return b

    pltpu.make_async_copy(x_ref.at[:, col(d, 256)], x_all.at[d], x_recv.at[d]).start()

    for n, (src, dst, width) in enumerate(pairs):

        for i, to in enumerate(farthest_first, 1):
            its_head = (to + 4 * gz) % GROUP
            remote(
                src.at[:, col(its_head, width)], dst.at[me],
                in_send.at[n, to], in_recv.at[n, me], (base + to, d),
            ).start()
            if n == 1:
                its = (d + i) % DPN
                remote(x_ref.at[:, col(its, 256)], x_all.at[d], x_send.at[its], x_recv.at[d], (s, its)).start()

    w_copy = pltpu.make_async_copy(w_ref, w_all, w_sem)
    w_copy.start()

    for r in range(2):
        arrived(rlam.at[r], lam_recv.at[r])
    row = lax.broadcasted_iota(jnp.int32, (BLOCK, BLOCK), 0)
    column = lax.broadcasted_iota(jnp.int32, (BLOCK, BLOCK), 1)
    ones = jnp.ones((BLOCK, BLOCK), F32)
    hi = lax.Precision.HIGHEST

    @pl.loop(0, GROUP)
    def _(b):
        kept = []
        for r in range(2):
            lam = jnp.broadcast_to(rlam[r, pl.ds(b, 1), :], (BLOCK, BLOCK))
            seen = column <= row if r == 0 else column >= row
            c = dot(jnp.where(seen, lam, 0.0), ones, 1, 0, hi)
            kept.append(c - c.T)
            end = c[BLOCK - 1 : BLOCK, :] if r == 0 else c[0:1, :]
            qs[r, b] = jnp.exp(c) * 0.0625
            ks[r, b] = jnp.exp(end - c)
            ee[r, b] = jnp.broadcast_to(end, (8, 128))
        wgt[b] = jnp.exp(jnp.where(column <= row, kept[0], kept[1])) * 0.0625

    for r in range(2):
        up = jnp.zeros((8, 128), F32)
        down = jnp.zeros((8, 128), F32)
        for b in range(GROUP):
            tails[r, 1, b] = jnp.exp(down)
            down = down + ee[r, b]
            tails[r, 0, GROUP - 1 - b] = jnp.exp(up)
            up = up + ee[r, GROUP - 1 - b]
        for b in range(GROUP):
            ee[r, b] = jnp.exp(ee[r, b])

    def order(i, way):
        return i + way * (GROUP - 1 - 2 * i)

    def send_state(st, n):
        st_tx[n] = st[...].astype(BF16)
        remote(st_tx.at[n], st_rx.at[n], st_send.at[n], st_recv.at[n], (partner, d)).start()

    def scaled(block, scale):
        return (block.astype(F32) * lanes(scale, DK)).astype(BF16)

    st[...] = jnp.zeros_like(st)

    @pl.loop(0, GROUP)
    def _(i):
        b = nth(i)
        for n in (0, 1):
            arrived(pairs[n][1].at[b], in_recv.at[n, b])
        st[...] += dot(scaled(rq[b], qs[1 - gz, b] * tails[1 - gz, gz, b][0:1, :]), rg[b], 0, 0)

    send_state(st, 0)

    def g_chain(way):
        r = 1 - way

        @pl.loop(0, GROUP)
        def _(i):
            b = order(i, way)
            g_all[r, b] = st[...].astype(BF16)
            st[...] = st[...] * lanes(ee[r, b][0:1, :], DV) + dot(scaled(rq[b], qs[r, b]), rg[b], 0, 0)

    st[...] = jnp.zeros_like(st)
    g_chain(gz)
    arrived(st_rx.at[0], st_recv.at[0])
    st[...] = st_rx[0].astype(F32)
    g_chain(1 - gz)

    homes = (
        (out_k, dk_all.at[d], DK),
        (out_v, dv_ref, DV),
        (out_q, dq_ref, DK),
    )

    def send_home(b, n):
        src, dst, width = homes[n]

        @pl.when(b == me)
        def _():
            pltpu.make_async_copy(src.at[b], dst.at[:, col(head, width)], out_recv.at[n, head]).start()

        @pl.when(b != me)
        def _():
            remote(
                src.at[b], dst.at[:, col(head, width)],
                out_send.at[n, b], out_recv.at[n, head], (base + b, d),
            ).start()

    @pl.loop(0, GROUP)
    def _(i):
        b = nth(i)
        arrived(rv.at[b], in_recv.at[2, b])
        v = rv[b]
        gs = (dot(rg[b], v, 1, 1) * wgt[b]).astype(BF16)
        gs_all[b] = gs
        dk = dot(gs, rq[b], 0, 0)
        for r in range(2):
            dk += dot(v, g_all[r, b], 1, 1) * lanes(ks[r, b], DK)
        out_k[b] = dk.astype(BF16)
        send_home(b, 0)

    st[...] = jnp.zeros_like(st)

    @pl.loop(0, GROUP)
    def _(i):
        b = nth(i)
        arrived(rk.at[b], in_recv.at[3, b])
        st[...] += dot(scaled(rk[b], ks[gz, b] * tails[gz, gz, b][0:1, :]), rv[b], 0, 0)

    send_state(st, 1)

    def piece(j, c):
        return dk_all.at[j, :, col(c, CHUNK)]

    left = 2 * ((xi + 3) % 4) + core
    right = 2 * ((xi + 1) % 4) + core
    across = 2 * ((xi + 2) % 4) + core

    def pass_on(j, c, sem, to):
        remote(piece(j, c), piece(j, c), sem, dk_recv.at[j, c], (s, to)).start()

    @pl.loop(0, GROUP)
    def _(i):
        b = nth(i)
        k = rk[b]
        dv = dot((dot(rq[b], k, 1, 1) * wgt[b]).astype(BF16), rg[b], 0, 0)
        for r in range(2):
            dv += dot(scaled(k, ks[r, b]), g_all[r, b], 1, 0)
        out_v[b] = dv.astype(BF16)
        send_home(b, 1)

        c = i // 2

        @pl.when(i % 2 == 0)
        def _():
            for h in range(CHUNK // DK):
                arrived(out_k.at[0], out_recv.at[0, c * (CHUNK // DK) + h])
            pass_on(d, c, dk_send.at[0, c], left)
            pass_on(d, c, dk_send.at[1, c], right)

        @pl.when(i % 2 == 1)
        def _():
            pass_on(d, c, dk_send.at[2, c], across)
            pass_on(d, c, dk_send.at[3, c], sibling)

    def m_step(b, r):
        dq = dot(rg[b], st[...].astype(BF16), 1, 1) * lanes(qs[r, b], DK)
        st[...] = st[...] * lanes(ee[r, b][0:1, :], DV) + dot(scaled(rk[b], ks[r, b]), rv[b], 0, 0)
        return dq

    st[...] = jnp.zeros_like(st)

    @pl.loop(0, GROUP)
    def _(i):
        b = order(i, gz)
        acc_q[b] = m_step(b, gz) + dot(gs_all[b], rk[b], 1, 0)

    @pl.loop(0, DPN)
    def _(j):
        arrived(x_all.at[j], x_recv.at[j])
        xt[:, col(j, BLOCK)] = x_all[j].T

    w_copy.wait()
    dx_acc[...] = jnp.zeros_like(dx_acc)

    arrived(st_rx.at[1], st_recv.at[1])
    st[...] = st_rx[1].astype(F32)

    @pl.loop(0, GROUP)
    def _(i):
        b = order(i, 1 - gz)
        out_q[b] = (acc_q[b] + m_step(b, 1 - gz)).astype(BF16)

    @pl.loop(0, GROUP)
    def _(i):
        send_home(nth(i), 2)

    sz, sy = s // 4, s % 4

    def axes(c):
        odd = c % 2
        one, two = sz + odd * (sy - sz), sy + odd * (sz - sy)

        def device(i, j):
            return (4 * i + j + odd * (3 * j - 3 * i), d)

        return one, two, device

    def rows(i, n):
        return pl.ds(pl.multiple_of(i * n, n), n)

    def first_sums(c):
        one, two, device = axes(c)
        pltpu.make_async_copy(dw_tx.at[c, rows(one, 64)], rx_one.at[c, one], sum_recv.at[0, c]).start()
        for t in range(1, 4):
            to = (one + t) % 4
            remote(
                dw_tx.at[c, rows(to, 64)], rx_one.at[c, one],
                sum_send.at[0, c], sum_recv.at[0, c], device(to, two),
            ).start()

    def second_sums(c):
        one, two, device = axes(c)
        arrived(rx_one.at[c], sum_recv.at[0, c])
        tx_two[c] = jnp.sum(rx_one[c].astype(F32), axis=0).astype(BF16)
        pltpu.make_async_copy(tx_two.at[c, rows(two, 16)], rx_two.at[c, two], sum_recv.at[1, c]).start()
        for t in range(1, 4):
            to = (two + t) % 4
            remote(
                tx_two.at[c, rows(to, 16)], rx_two.at[c, two],
                sum_send.at[1, c], sum_recv.at[1, c], device(one, to),
            ).start()

    def first_back(c):
        one, two, device = axes(c)
        arrived(rx_two.at[c], sum_recv.at[1, c])
        sum_tx[c] = jnp.sum(rx_two[c].astype(F32), axis=0).astype(BF16)
        place = dw_sum.at[c, rows(4 * one + two, 16)]
        pltpu.make_async_copy(sum_tx.at[c], place, sum_recv.at[2, c]).start()
        for t in range(1, 4):
            remote(
                sum_tx.at[c], place, sum_send.at[2, c], sum_recv.at[2, c], device(one, (two + t) % 4)
            ).start()

    def second_back(c):
        one, two, device = axes(c)
        place = dw_sum.at[c, rows(one, 64)]
        arrived(place, sum_recv.at[2, c])
        for t in range(1, 4):
            remote(place, place, sum_send.at[3, c], sum_recv.at[3, c], device((one + t) % 4, two)).start()

    def last_sums():
        pltpu.make_async_copy(dw_tx.at[LAST, rows(s, 16)], dw_rx.at[s], last_recv.at[0]).start()

        @pl.loop(1, SP)
        def _(i):
            to = (s + i) % SP
            remote(
                dw_tx.at[LAST, rows(to, 16)], dw_rx.at[s], last_send.at[0], last_recv.at[0], (to, d)
            ).start()

    def last_back():
        arrived(dw_rx, last_recv.at[0])
        sum_tx[LAST] = jnp.sum(dw_rx[...].astype(F32), axis=0).astype(BF16)
        place = dw_sum.at[LAST, rows(s, 16)]
        pltpu.make_async_copy(sum_tx.at[LAST], place, last_recv.at[1]).start()

        @pl.loop(1, SP)
        def _(i):
            remote(
                sum_tx.at[LAST], place, last_send.at[1], last_recv.at[1], ((s + i) % SP, d)
            ).start()

    def follow_up(i):
        for n, work in enumerate((second_sums, first_back, second_back)):
            c = i - 1 - n

            if not isinstance(c, int):

                @pl.when(jnp.logical_and(c >= 0, c < LAST))
                def _():
                    work(c)

            elif c < LAST:
                work(c)

    def gathered(c):
        for n, j in enumerate((left, right, across)):
            arrived(piece(j, c), dk_recv.at[j, c])
            pass_on(j, c, dk_fwd.at[n, c], sibling)
        for j in range(4):
            far = 2 * ((xi + j) % 4) + 1 - core
            arrived(piece(far, c), dk_recv.at[far, c])
        part = dk_all[:, :, col(c, CHUNK)].reshape(DPN * BLOCK, CHUNK)
        dw_tx[c] = dot(xt[...], part, 1, 0).astype(BF16)
        return part

    @pl.loop(0, LAST)
    def _(c):
        part = gathered(c)
        first_sums(c)
        dx_acc[...] += dot(part, w_all[:, col(c, CHUNK)], 1, 1)
        follow_up(c)

    part = gathered(LAST)
    last_sums()
    columns = dx_ref.at[:, col(d, 256)]
    dx_st[...] = (dx_acc[...] + dot(part, w_all[:, col(LAST, CHUNK)], 1, 1)).astype(BF16).reshape(DPN, BLOCK, 256)
    pltpu.make_async_copy(dx_st.at[d], columns, dx_recv.at[d]).start()

    @pl.loop(1, DPN)
    def _(i):
        to = (d + i) % DPN
        remote(dx_st.at[to], columns, dx_send.at[to], dx_recv.at[d], (s, to)).start()

    follow_up(LAST)
    follow_up(CHUNKS)
    last_back()
    follow_up(CHUNKS + 1)

    @pl.loop(0, GROUP)
    def _(h):
        arrived(out_v.at[h], out_recv.at[1, h])
        arrived(out_q.at[h], out_recv.at[2, h])

    @pl.loop(0, DPN)
    def _(j):
        arrived(dx_st.at[j], dx_recv.at[j])

    for half in range(2):

        @pl.when(lam_to[half] != s)
        def _():
            arrived(rlam.at[half], lam_send.at[half])

    @pl.loop(1, GROUP)
    def _(i):
        to = (me + i) % GROUP
        for n, (_, dst, _) in enumerate(pairs):
            arrived(dst.at[to], in_send.at[n, to])
        for n, (src, _, _) in enumerate(homes):
            arrived(src.at[to], out_send.at[n, to])

    @pl.loop(1, DPN)
    def _(i):
        to = (d + i) % DPN
        arrived(x_all.at[to], x_send.at[to])
        arrived(dx_st.at[to], dx_send.at[to])

    for n in range(2):
        arrived(st_tx.at[n], st_send.at[n])

    @pl.loop(0, CHUNKS)
    def _(c):
        own = piece(d, c)
        for t in range(4):
            arrived(own, dk_send.at[t, c])
        for t in range(3):
            arrived(own, dk_fwd.at[t, c])

    @pl.loop(0, LAST)
    def _(c):
        arrived(rx_one.at[c, pl.ds(0, 3)], sum_send.at[0, c])
        arrived(rx_two.at[c, pl.ds(0, 3)], sum_send.at[1, c])
        arrived(rx_two.at[c, pl.ds(0, 3)], sum_send.at[2, c])
        three = dw_sum.at[c, pl.ds(0, 192)]
        arrived(three, sum_send.at[3, c])
        arrived(three, sum_recv.at[3, c])
        dw_ref[:, col(c, CHUNK)] = dw_sum[c].astype(F32)

    for n in range(2):
        arrived(dw_rx.at[pl.ds(0, SP - 1)], last_send.at[n])
    arrived(dw_sum.at[LAST], last_recv.at[1])
    dw_ref[:, col(LAST, CHUNK)] = dw_sum[LAST].astype(F32)


def write_out(*refs):
    sems = refs[-1]
    copies = [pltpu.make_async_copy(refs[n], refs[n + 4], sems.at[n]) for n in range(4)]
    for copy in copies:
        copy.start()
    for copy in copies:
        copy.wait()


def step(x, q, k, v, g, lam, w):
    vmem = pl.BlockSpec(memory_space=pltpu.VMEM)
    hbm = pl.BlockSpec(memory_space=pl.ANY)
    dma = pltpu.SemaphoreType.DMA
    v_ = pltpu.VMEM
    results = pl.pallas_call(
        kernel,
        out_shape=(
            v_((BLOCK, 2048), BF16), v_((BLOCK, 4096), BF16), v_((BLOCK, 2048), BF16), v_((256, 2048), F32)
        ),
        in_specs=[hbm, hbm, hbm, hbm, hbm, vmem, hbm],
        out_specs=(vmem,) * 4,
        scratch_shapes=[
            v_((8, BLOCK, DK), BF16), v_((8, BLOCK, DK), BF16),
            v_((8, BLOCK, DV), BF16), v_((8, BLOCK, DV), BF16),
            v_((2, 8, 128), F32), v_((256, 2048), BF16), v_((8, BLOCK, 256), BF16),
            v_((2, 8, BLOCK, 128), F32), v_((2, 8, BLOCK, 128), F32),
            v_((2, 8, 8, 128), F32), v_((2, 2, 8, 8, 128), F32), v_((8, BLOCK, 128), F32),
            v_((8, BLOCK, DK), F32), v_((8, BLOCK, BLOCK), BF16), v_((2, 8, DK, DV), BF16),
            v_((DK, DV), F32), v_((2, DK, DV), BF16), v_((2, DK, DV), BF16),
            v_((8, BLOCK, DK), BF16), v_((8, BLOCK, DK), BF16), v_((8, BLOCK, DV), BF16),
            v_((8, BLOCK, D), BF16), v_((8, BLOCK, 256), BF16), v_((8 * BLOCK, 256), F32),
            v_((256, 8 * BLOCK), BF16), v_((CHUNKS, 256, CHUNK), BF16),
            v_((LAST, 4, 64, CHUNK), BF16), v_((LAST, 64, CHUNK), BF16), v_((LAST, 4, 16, CHUNK), BF16),
            v_((16, 16, CHUNK), BF16),
            v_((CHUNKS, 16, CHUNK), BF16), v_((CHUNKS, 256, CHUNK), BF16),
            dma((4, 8)), dma((4, 8)), dma((2,)), dma((2,)), dma((8,)), dma((8,)), dma,
            dma((2,)), dma((2,)), dma((3, 8)), dma((3, 8)),
            dma((4, CHUNKS)), dma((3, CHUNKS)), dma((8, CHUNKS)), dma((8,)), dma((8,)),
            dma((4, LAST)), dma((4, LAST)), dma((2,)), dma((2,)),
        ],
        compiler_params=pltpu.CompilerParams(
            collective_id=0, has_side_effects=True, vmem_limit_bytes=58 * 1024 * 1024
        ),
    )(x[0], q[0], k[0], v[0], g[0], lam[0].reshape(16, 128), w)
    dq, dv, dx, dw = pl.pallas_call(
        write_out,
        out_shape=tuple(pltpu.HBM(a.shape, a.dtype) for a in results),
        in_specs=[hbm] * 4,
        out_specs=(hbm,) * 4,
        scratch_shapes=[dma((4,))],
        compiler_params=pltpu.CompilerParams(vmem_limit_bytes=20 * 1024 * 1024),
    )(*results)
    return dq[None], dv[None], dx[None], dw


def solution(mesh):
    tokens = P("dp", "sp", None)
    return jax.shard_map(
        step,
        mesh=mesh,
        in_specs=(tokens,) * 6 + (P("dp", None),),
        out_specs=(tokens, tokens, tokens, P("dp", None)),
        check_vma=False,
    )
```
